256 devices in a mesh: sp: 64 (over z, y, core), tp: 4 (over x).
Axes of the slice: x: 4, y: 4, z: 8, core: 2. Of those that a mesh axis runs over, the one named last changes fastest.
Arguments:
- tokens: bfloat16 [65536, 2048], P('sp', 'tp'), may hold values from -600 to 600, as said below
- norm_gain: float32 [2048], replicated, may hold values from 0.1 to 1.9
- w_query: bfloat16 [2048, 1024], P(None, 'tp'), may hold values from -0.125 to 0.125
- w_forget_fwd: bfloat16 [2048, 1024], P(None, 'tp'), may hold values from -0.125 to 0.125
- w_forget_bwd: bfloat16 [2048, 1024], P(None, 'tp'), may hold values from -0.125 to 0.125
- w_value: bfloat16 [2048, 1024], P(None, 'tp'), may hold values from -0.125 to 0.125
- w_gate: bfloat16 [2048, 1024], P(None, 'tp'), may hold values from -0.125 to 0.125
- w_pool_in: bfloat16 [2048, 1024], P(None, 'tp'), may hold values from -0.125 to 0.125
- forget_gap: float32 [2, 1024], P(None, 'tp'), may hold values from 0 to 0.06
- added_log_retention: float32 [65536, 8], P('sp', 'tp'), may hold values from -2.1 to 0
- initial_state: float32 [2, 8, 128, 128], P(None, 'tp'), may hold values from -0.18 to 0.18
- head_gain: float32 [1024], P('tp'), may hold values from 0.1 to 1.9
- pool_mix: bfloat16 [4, 256, 256], P('tp'), may hold values from -0.375 to 0.375
- pool_gain: float32 [1024], P('tp'), may hold values from 0.1 to 1.9
- w_out_recur: bfloat16 [1024, 2048], P('tp'), may hold values from -0.125 to 0.125
- w_out_pool: bfloat16 [1024, 2048], P('tp'), may hold values from -0.125 to 0.125
Outputs:
- mixed_out: bfloat16 [65536, 2048], P(('sp', 'tp'))
The draws below stay inside these ranges and needn't reach their ends.
Inputs may be any that keep to these rules, and one draw needn't show every extreme that they name: `tokens`: layer input with scales that differ between rows and between columns.
All inputs are finite; a program needn't handle non-finite values.
Results may differ from the reference program's by a relative error of at most 0.013.
Values may be sent and summed in bfloat16 or wider, within the bound.
No kernel may reach another device: no remote copies, remote signals or barrier semaphores. Data moves between devices by JAX's collectives and lax.ppermute only.
A program may use at most 128 MiB of HBM per device.

```python
import jax
import jax.numpy as jnp
from jax import lax

D = 2048
HEADS = 8
HEAD_DIM = 128
EXPAND = 128
POOL_GROUPS = 4
POOL_GROUP = 256
BLOCK = 64
TOK_DEV = 1024
SEQ = 65536
HG_WIDTH = 1024
KDIM = 1024
POOL_WIDTH = 1024
N_TP = 4


def draw_tokens(key, part):
    first, second, third = jax.random.split(key, 3)
    base = jnp.clip(jax.random.normal(first, (SEQ, D), jnp.float32), -6.0, 6.0)
    row_scale = 10.0 ** jax.random.uniform(second, (SEQ, 1), jnp.float32, 0.0, 1.0)
    rising = jnp.arange(D, dtype=jnp.float32) / D
    column_scale = 10.0 ** (0.8 * rising + jax.random.uniform(third, (1, D), jnp.float32, 0.0, 0.2))
    return (base * row_scale * column_scale).astype(jnp.bfloat16)


def draw_forget_gap(key, part):
    pick_key, fast_key, slow_key = jax.random.split(key, 3)
    share = 0.5
    fast_heads = jax.random.uniform(pick_key, (2, HEADS, 1), jnp.float32) < share
    fast_gap = jax.random.uniform(fast_key, (2, HEADS, EXPAND), jnp.float32, 0.02, 0.06)
    lowest = jnp.log(jnp.float32(0.3 / SEQ))
    highest = jnp.log(jnp.float32(min(30.0 / SEQ, 0.06)))
    slow_gap = jnp.exp(jax.random.uniform(slow_key, (2, HEADS, EXPAND), jnp.float32, lowest, highest))
    return jnp.where(fast_heads, fast_gap, slow_gap).reshape(2, HEADS * EXPAND)


def draw_added_log_retention(key, part):
    level_key, where_key, size_key = jax.random.split(key, 3)
    span = max(TOK_DEV // 4, 1)
    pieces = SEQ // span
    lowest = jnp.log(jnp.float32(0.1 / SEQ))
    highest = jnp.log(jnp.float32(1.0 / SEQ))
    level = jnp.exp(jax.random.uniform(level_key, (pieces, 1, HEADS), jnp.float32, lowest, highest))
    backdrop_term = -jnp.broadcast_to(level, (pieces, span, HEADS)).reshape(SEQ, HEADS)
    spots = jax.random.randint(where_key, (3, HEADS), 0, SEQ)
    layer_depth = jax.random.uniform(size_key, (3, HEADS), jnp.float32, 0.22, 0.69)
    location_list = jnp.arange(SEQ, dtype=jnp.int32)[:, None, None] == spots[None, :, :]
    token_groups = -jnp.sum(jnp.where(location_list, layer_depth[None, :, :], 0.0), axis=1)
    return backdrop_term + token_groups


def steps_of(rng, shape, cuts, low, largest):
    loudness = 1.0
    for dim, parts in cuts:
        heights = jax.random.uniform(jax.random.fold_in(jax.random.fold_in(rng, 6), dim), (parts,), jnp.float32, low / len(cuts), largest / len(cuts))
        loudness = loudness * jnp.repeat(jnp.exp(heights), shape[dim] // parts).reshape((-1,) + (1,) * (len(shape) - 1 - dim))
    return loudness


def normal_values(rng, dims, deviation, most, shards=(), kind=jnp.bfloat16):
    factor_of = steps_of(rng, dims, shards, -0.22, 0.18) if shards else 1.0
    values = jax.random.normal(rng, dims, jnp.float32) * deviation * factor_of
    return jnp.minimum(jnp.maximum(values, -most), most).astype(kind)


def setup_inputs(seed: int = 0) -> dict:
    streams_of = jax.random.split(jax.random.key(seed), 17)
    return {
        "tokens": draw_tokens(jax.random.fold_in(streams_of[16], 71), 0),
        "norm_gain": jnp.clip(1.0 + 0.18 * jax.random.normal(streams_of[1], (D,), jnp.float32), 0.1, 1.9),
        "w_query": normal_values(streams_of[2], (D, KDIM), D ** -0.5, 0.125, ((1, 4),)),
        "w_forget_fwd": normal_values(streams_of[3], (D, KDIM), D ** -0.5, 0.125, ((1, 4),)),
        "w_forget_bwd": normal_values(streams_of[4], (D, KDIM), D ** -0.5, 0.125, ((1, 4),)),
        "w_value": normal_values(streams_of[5], (D, HG_WIDTH), D ** -0.5, 0.125, ((1, 4),)),
        "w_gate": normal_values(streams_of[6], (D, HG_WIDTH), D ** -0.5, 0.125, ((1, 4),)),
        "w_pool_in": normal_values(streams_of[7], (D, POOL_WIDTH), D ** -0.5, 0.125, ((1, 4),)),
        "forget_gap": draw_forget_gap(jax.random.fold_in(streams_of[16], 71), 0),
        "added_log_retention": draw_added_log_retention(jax.random.fold_in(streams_of[16], 71), 0),
        "initial_state": normal_values(streams_of[10], (2, HEADS, EXPAND, HEAD_DIM), 0.03, 0.18, ((1, 4),), jnp.float32),
        "head_gain": jnp.clip(1.0 + 0.18 * jax.random.normal(streams_of[11], (HG_WIDTH,), jnp.float32), 0.1, 1.9),
        "pool_mix": normal_values(streams_of[12], (POOL_GROUPS, POOL_GROUP, POOL_GROUP), POOL_GROUP ** -0.5, 0.375, ((0, 4),)),
        "pool_gain": jnp.clip(1.0 + 0.18 * jax.random.normal(streams_of[13], (POOL_WIDTH,), jnp.float32), 0.1, 1.9),
        "w_out_recur": normal_values(streams_of[14], (HG_WIDTH, D), (HG_WIDTH + POOL_WIDTH) ** -0.5, 0.125, ((0, 4),)),
        "w_out_pool": normal_values(streams_of[15], (POOL_WIDTH, D), (HG_WIDTH + POOL_WIDTH) ** -0.5, 0.125, ((0, 4),)),
    }


EPSILON = 1e-06
FULL_ACCURACY = lax.Precision.HIGHEST

def project(normed, scale, weight):
    return (jnp.dot(normed, weight, preferred_element_type=jnp.float32) * scale).astype(jnp.bfloat16)

def recurrence(query, block_entry, values, log_keep, start):
    length, heads, layer_depth = query.shape
    count = length // BLOCK

    def split(array):
        return array.reshape(count, BLOCK, heads, array.shape[2]).transpose(0, 2, 1, 3)
    lower = jnp.tril(jnp.ones((BLOCK, BLOCK), jnp.float32))

    def advance(hidden_state, inputs):
        query_block, entry_block, value_tile_rows, keep_block = inputs
        running = jnp.cumsum(keep_block, axis=1)
        query_retention = query_block * jnp.exp(running)
        entry_decay = entry_block * jnp.exp(-running)
        scores = jnp.einsum('hck,hsk->hcs', query_retention, entry_decay, precision=FULL_ACCURACY) * lower
        final_output = jnp.einsum('hcs,hsv->hcv', scores, value_tile_rows, precision=FULL_ACCURACY)
        final_output = final_output + jnp.einsum('rbl,rlm->rbm', query_retention, hidden_state, precision=FULL_ACCURACY)
        closing_value = running[:, -1:, :]
        final_block_entry = entry_block * jnp.exp(closing_value - running)
        hidden_state = jnp.exp(closing_value[:, 0, :, None]) * hidden_state + jnp.einsum('xnw,xnz->xwz', final_block_entry, value_tile_rows, precision=FULL_ACCURACY)
        return (hidden_state, final_output)
    hidden_state, final_output = lax.scan(advance, start, (split(query), split(block_entry), split(values), split(log_keep)))
    return final_output.transpose(0, 2, 1, 3).reshape(length, heads, values.shape[2])

def reference(tokens, norm_gain, w_query, w_forget_fwd, w_forget_bwd, w_value, w_gate, w_pool_in, forget_gap, added_log_retention, initial_state, head_gain, pool_mix, pool_gain, w_out_recur, w_out_pool):
    widened = tokens.astype(jnp.float32)
    scale = lax.rsqrt(lax.optimization_barrier(jnp.mean(widened * widened, axis=1, keepdims=True)) + EPSILON)
    normed = (widened * norm_gain).astype(jnp.bfloat16)
    query_pre = project(normed, scale, w_query)
    forget_fwd = project(normed, scale, w_forget_fwd)
    forget_bwd = project(normed, scale, w_forget_bwd)
    value_proj = project(normed, scale, w_value)
    gate_pre = project(normed, scale, w_gate)
    pool_in = project(normed, scale, w_pool_in)

    def split_heads(array, width):
        return array.astype(jnp.float32).reshape(SEQ, HEADS, width)
    query = jax.nn.silu(split_heads(query_pre, EXPAND))
    values = split_heads(value_proj, HEAD_DIM)
    token_group = added_log_retention[:, :, None]

    def gates(pre, gap):
        block_entry = gap.reshape(HEADS, EXPAND) * jax.nn.sigmoid(-split_heads(pre, EXPAND))
        return (block_entry, jnp.log1p(-block_entry) + token_group)
    entry_fwd, keep_fwd = gates(forget_fwd, forget_gap[0])
    entry_bwd, keep_bwd = gates(forget_bwd, forget_gap[1])
    out_fwd = recurrence(query, entry_fwd, values, keep_fwd, initial_state[0])
    output_backward = jnp.flip(recurrence(jnp.flip(query, 0), jnp.flip(entry_bwd, 0), jnp.flip(values, 0), jnp.flip(keep_bwd, 0), initial_state[1]), 0)
    both = out_fwd + output_backward
    both = both * lax.rsqrt(lax.optimization_barrier(jnp.mean(both * both, axis=2, keepdims=True)) + EPSILON)
    recur = (both.reshape(SEQ, HG_WIDTH) * head_gain * jax.nn.sigmoid(gate_pre.astype(jnp.float32))).astype(jnp.bfloat16)
    positions = jnp.arange(SEQ, dtype=jnp.int32)
    pooled = []
    for group in range(POOL_GROUPS):
        window = 2 ** (group + 1)
        current = pool_in[:, group * POOL_GROUP:(group + 1) * POOL_GROUP].astype(jnp.float32)
        sums = jnp.concatenate([jnp.zeros((1, POOL_GROUP), jnp.float32), jnp.cumsum(current, axis=0)], axis=0)
        low = jnp.clip(positions - window // 2, 0, SEQ)
        high = jnp.clip(positions - window // 2 + window, 0, SEQ)
        window_mean = (sums[high] - sums[low]) / (high - low).astype(jnp.float32)[:, None]
        diff = (window_mean - current).astype(jnp.bfloat16)
        pooled.append(jnp.dot(diff, pool_mix[group], preferred_element_type=jnp.float32))
    pool_out = (jnp.concatenate(pooled, axis=1) * pool_gain).astype(jnp.bfloat16)
    recur_share = HG_WIDTH // N_TP
    pool_share = POOL_WIDTH // N_TP
    total = jnp.zeros((SEQ, D), jnp.float32)
    for rank in range(N_TP):
        partial_sum = jnp.dot(recur[:, rank * recur_share:(rank + 1) * recur_share], w_out_recur[rank * recur_share:(rank + 1) * recur_share], preferred_element_type=jnp.float32)
        partial_sum = partial_sum + jnp.dot(pool_out[:, rank * pool_share:(rank + 1) * pool_share], w_out_pool[rank * pool_share:(rank + 1) * pool_share], preferred_element_type=jnp.float32)
        rounded = lax.optimization_barrier(partial_sum.astype(jnp.bfloat16))
        total = total + rounded.astype(jnp.float32)
    return total.astype(jnp.bfloat16)
```

```python
import jax
import jax.numpy as jnp
from jax import lax
from jax.experimental import pallas as pl
from jax.experimental.pallas import tpu as pltpu
from jax.sharding import Mesh
from jax.sharding import PartitionSpec as P

D = 2048
HEADS = 2
K = 128
TILE = 256
BLOCK = 64
PER_TILE = TILE // BLOCK
CHUNKS = ((0, 768), (768, 256))
RIM = 8
PAD = 64
EPSILON = 1e-06
F32 = jnp.float32
BF16 = jnp.bfloat16


def nt(a, b):
    return lax.dot_general(a, b, (((1,), (1,)), ((), ())), preferred_element_type=F32)


def tn(a, b):
    return lax.dot_general(a, b, (((0,), (0,)), ((), ())), preferred_element_type=F32)


def nn(a, b):
    return jnp.dot(a, b, preferred_element_type=F32)


def parts_of(x):
    hi = x.astype(BF16)
    rest = x - hi.astype(F32)
    mid = rest.astype(BF16)
    return hi, mid, (rest - mid.astype(F32)).astype(BF16)


def project_kernel(
    tp, own, left, right, far_a, far_b, gain, wq, wf, wb, wv, wg, wp, gap, added, state_in, total_in,
    q_out, k_out, v_out, gate_out, pool_out, kv_out, close_out, state_out, total_out, message_out,
):
    step = pl.program_id(0)

    @pl.when(step == 0)
    def _():
        state_out[...] = state_in[...]
        total_out[...] = total_in[...]

    me = tp[0]
    squares = jnp.zeros((TILE, 128), F32)
    normed = []
    for ref, shift, at in ((own, 0, 0), (left, 3, 0), (right, 1, 0), (far_a, 2, 0), (far_b, 2, 256)):
        group = lax.rem(me + shift, 4)
        width = ref.shape[1]
        x = ref[...].astype(F32)
        for c in range(0, width, 128):
            squares = squares + x[:, c : c + 128] * x[:, c : c + 128]
        normed.append(((x * gain[group][:, at : at + width]).astype(BF16), pl.multiple_of(group * 512 + at, 256), width))
    scale = lax.rsqrt(jnp.sum(squares, axis=1, keepdims=True) / D + EPSILON)

    def projected(w):
        total = None
        for n, at, width in normed:
            piece = nn(n, w[pl.ds(at, width), :])
            total = piece if total is None else total + piece
        return (total * scale).astype(BF16)

    value = projected(wv)
    v_out[...] = value
    query_pre = projected(wq).astype(F32)
    query = query_pre / (1.0 + jnp.exp(-query_pre))
    row = lax.broadcasted_iota(jnp.int32, (TILE, TILE), 0)
    col = lax.broadcasted_iota(jnp.int32, (TILE, TILE), 1)
    same = (row // BLOCK) == (col // BLOCK)
    adds = jnp.concatenate([jnp.broadcast_to(added[:, h : h + 1], (TILE, K)) for h in range(HEADS)], axis=1)
    ends = []
    closes = []
    for d, w in ((0, wf), (1, wb)):
        pre = projected(w).astype(F32)
        enter = gap[d : d + 1, :] / (1.0 + jnp.exp(pre))
        series = 1.0 / 7.0
        for n in (6, 5, 4, 3, 2):
            series = series * enter + 1.0 / n
        keep = adds - enter * (series * enter + 1.0)
        sums = jnp.where(same & ((col <= row) if d == 0 else (col >= row)), 1.0, 0.0).astype(BF16)
        hi, mid, lo = parts_of(keep)
        running = nn(sums, hi) + (nn(sums, mid) + nn(sums, lo))
        close = [running[b * BLOCK + (BLOCK - 1) * (1 - d) :][:1] for b in range(PER_TILE)]
        closing = jnp.concatenate([jnp.broadcast_to(c, (BLOCK, c.shape[1])) for c in close], axis=0)
        q = (query * jnp.exp(running)).astype(BF16)
        k = (enter * jnp.exp(-running)).astype(BF16)
        for h in range(HEADS):
            to = (2 * h + d) * K
            q_out[:, to : to + K] = q[:, h * K : (h + 1) * K]
            k_out[:, to : to + K] = k[:, h * K : (h + 1) * K]
        ends.append((enter * jnp.exp(closing - running)).astype(BF16))
        closes.append(close)
    gate_out[...] = projected(wg)
    pool_out[...] = projected(wp)
    for b in range(PER_TILE):
        rows = slice(b * BLOCK, (b + 1) * BLOCK)
        for h in range(HEADS):
            lanes = slice(h * K, (h + 1) * K)
            kv = tn(value[rows, lanes], jnp.concatenate([ends[0][rows, lanes], ends[1][rows, lanes]], axis=1))
            kv_out[b, h] = kv.astype(BF16)
            cf, cb = closes[0][b][:, lanes], closes[1][b][:, lanes]
            total = total_out[h]
            old = jnp.concatenate([jnp.exp(cf), jnp.ones_like(cb)], axis=1)
            new = jnp.concatenate([jnp.ones_like(cf), jnp.exp(total[:, K:])], axis=1)
            state_out[h] = old * state_out[h] + new * kv
            both = jnp.concatenate([cf, cb], axis=1)
            close_out[b, h] = both
            total_out[h] = total + both

    @pl.when(step == pl.num_programs(0) - 1)
    def _():
        pieces = []
        for p in zip(*(parts_of(total_out[h]) for h in range(HEADS))):
            pieces += [x.astype(F32) for x in p]
        tail = jnp.concatenate(pieces + [jnp.zeros((10, 2 * K), F32)], axis=0).astype(BF16)
        for g in range(8):
            for h in range(HEADS):
                message_out[g, h * 16 : (h + 1) * 16, :] = state_out[h, g * 16 : (g + 1) * 16, :].astype(BF16)
            message_out[g, 32:48, :] = tail


def project(tp, tokens, gain, weights, gap, added, state, total):
    rows = added.shape[0]
    steps = rows // TILE
    whole = lambda a: pl.BlockSpec(a.shape, lambda i: (0,) * a.ndim)
    tile = lambda a: pl.BlockSpec((TILE, a.shape[1]), lambda i: (i, 0))
    return pl.pallas_call(
        project_kernel,
        grid=(steps,),
        in_specs=[pl.BlockSpec(memory_space=pltpu.SMEM)]
        + [tile(t) for t in tokens]
        + [whole(gain)]
        + [whole(w) for w in weights]
        + [whole(gap), tile(added), whole(state), whole(total)],
        out_specs=[
            pl.BlockSpec((TILE, 512), lambda i: (i, 0)),
            pl.BlockSpec((TILE, 512), lambda i: (i, 0)),
            pl.BlockSpec((TILE, 256), lambda i: (i, 0)),
            pl.BlockSpec((TILE, 256), lambda i: (i, 0)),
            pl.BlockSpec((TILE, 256), lambda i: (i, 0)),
            pl.BlockSpec((PER_TILE, HEADS, K, 2 * K), lambda i: (i, 0, 0, 0)),
            pl.BlockSpec((PER_TILE, HEADS, 1, 2 * K), lambda i: (i, 0, 0, 0)),
            whole(state),
            whole(total),
            pl.BlockSpec((8, 48, 256), lambda i: (0, 0, 0)),
        ],
        out_shape=[
            jax.ShapeDtypeStruct((rows, 512), BF16),
            jax.ShapeDtypeStruct((rows, 512), BF16),
            jax.ShapeDtypeStruct((rows, 256), BF16),
            jax.ShapeDtypeStruct((rows, 256), BF16),
            jax.ShapeDtypeStruct((rows, 256), BF16),
            jax.ShapeDtypeStruct((rows // BLOCK, HEADS, K, 2 * K), BF16),
            jax.ShapeDtypeStruct((rows // BLOCK, HEADS, 1, 2 * K), F32),
            jax.ShapeDtypeStruct(state.shape, F32),
            jax.ShapeDtypeStruct(total.shape, F32),
            jax.ShapeDtypeStruct((8, 48, 256), BF16),
        ],
        compiler_params=pltpu.CompilerParams(dimension_semantics=("arbitrary",), vmem_limit_bytes=40 * 2**20),
        name="project",
    )(tp, *tokens, gain, *weights, gap, added, state, total)


def local_kernel(place, q, k, v, padded, mix, gain, out, pooled):
    step = pl.program_id(0)
    row = lax.broadcasted_iota(jnp.int32, (TILE, TILE), 0)
    col = lax.broadcasted_iota(jnp.int32, (TILE, TILE), 1)
    same = (row // BLOCK) == (col // BLOCK)
    ahead, behind = same & (col <= row), same & (col >= row)
    for h in range(HEADS):
        f = slice(2 * h * K, (2 * h + 1) * K)
        b = slice((2 * h + 1) * K, (2 * h + 2) * K)
        scores = jnp.where(ahead, nt(q[:, f], k[:, f]), 0.0) + jnp.where(behind, nt(q[:, b], k[:, b]), 0.0)
        out[:, h * K : (h + 1) * K] = nn(scores.astype(BF16), v[:, h * K : (h + 1) * K])
    group, first, sequence = place[0], place[1], place[2]
    window = jnp.left_shift(jnp.int32(2), group)
    span = TILE + 2 * PAD
    base = first + step * TILE
    target = base + lax.broadcasted_iota(jnp.int32, (TILE, span), 0)
    source = base - PAD + lax.broadcasted_iota(jnp.int32, (TILE, span), 1)
    low = target - jnp.right_shift(window, 1)
    inside = (source >= low) & (source < low + window) & (source >= 0) & (source < sequence)
    near = padded[pl.ds(pl.multiple_of(step * TILE, TILE), span), :]
    one = base + lax.broadcasted_iota(jnp.int32, (TILE, 1), 0)
    start = one - jnp.right_shift(window, 1)
    count = (jnp.minimum(start + window, sequence) - jnp.maximum(start, 0)).astype(F32)
    mean = nn(jnp.where(inside, 1.0, 0.0).astype(BF16), near) / count
    diff = (mean - near[PAD : PAD + TILE].astype(F32)).astype(BF16)
    pooled[...] = (nn(diff, mix[...]) * gain[...]).astype(BF16)


def local(place, q, k, v, padded, mix, gain):
    rows = q.shape[0]
    whole = lambda a: pl.BlockSpec(a.shape, lambda i: (0,) * a.ndim)
    tile = lambda a: pl.BlockSpec((TILE, a.shape[1]), lambda i: (i, 0))
    return pl.pallas_call(
        local_kernel,
        grid=(rows // TILE,),
        in_specs=[pl.BlockSpec(memory_space=pltpu.SMEM), tile(q), tile(k), tile(v), whole(padded), whole(mix), whole(gain)],
        out_specs=[tile(v), tile(v)],
        out_shape=[jax.ShapeDtypeStruct(v.shape, F32), jax.ShapeDtypeStruct(v.shape, BF16)],
        compiler_params=pltpu.CompilerParams(dimension_semantics=("arbitrary",), vmem_limit_bytes=24 * 2**20),
        name="local",
    )(place, q, k, v, padded, mix, gain)


def total_rows(message, h):
    return sum(message[32 + 2 * n + h : 33 + 2 * n + h].astype(F32) for n in (2, 1, 0))


def twice(rows):
    return jnp.concatenate([jnp.broadcast_to(r, (16, r.shape[1])) for r in rows], axis=0)


def group_kernel(got, prefix, reach, message):
    tiles = [got[g].astype(F32) for g in range(8)]
    totals = [[total_rows(t, h) for h in range(HEADS)] for t in tiles]
    f, b = slice(0, K), slice(K, 2 * K)
    summed = [None, None]
    spans = [None, None]
    for d, lanes, order in ((0, f, range(8)), (1, b, range(7, -1, -1))):
        state = jnp.zeros((32, K), F32)
        span = [jnp.zeros((1, K), F32)] * HEADS
        for g in order:
            prefix[g, :, lanes] = state
            reach[g, :, lanes] = jnp.exp(twice(span))
            here = [totals[g][h][:, lanes] for h in range(HEADS)]
            state = jnp.exp(twice(here)) * state + tiles[g][:32, lanes]
            span = [s + t for s, t in zip(span, here)]
        summed[d], spans[d] = state, span
    message[0:32, :] = jnp.concatenate(summed, axis=1).astype(BF16)
    pieces = []
    for p in zip(*(parts_of(jnp.concatenate([spans[0][h], spans[1][h]], axis=1)) for h in range(HEADS))):
        pieces += [x.astype(F32) for x in p]
    message[32:48, :] = jnp.concatenate(pieces + [jnp.zeros((10, 2 * K), F32)], axis=0).astype(BF16)


def cross_kernel(place, got, prefix, reach, initial, arriving):
    me = place[0]
    f, b = slice(0, K), slice(K, 2 * K)
    tiles = [got[z].astype(F32) for z in range(8)]
    for d, lanes, order in ((0, f, range(8)), (1, b, range(7, -1, -1))):
        state = initial[:, lanes]
        for z in order:
            here = [total_rows(tiles[z], h)[:, lanes] for h in range(HEADS)]
            moved = jnp.exp(twice(here)) * state + tiles[z][:32, lanes]
            state = jnp.where((z < me) if d == 0 else (z > me), moved, state)
        for g in range(8):
            arriving[g, :, lanes] = (prefix[g, :, lanes] + reach[g, :, lanes] * state).astype(BF16)


def finish_kernel(arriving, kv, close, q, out, gate, gain, recur, states):
    step = pl.program_id(0)
    blocks = kv.shape[0]

    @pl.when(step == 0)
    def _():
        for h in range(HEADS):
            came = jnp.concatenate([arriving[g, h * 16 : (h + 1) * 16, :] for g in range(8)], axis=0).astype(F32)
            for d in range(2):
                lanes = slice(d * K, (d + 1) * K)

                def advance(i, state):
                    b = i if d == 0 else blocks - 1 - i
                    states[b, h, :, lanes] = state.astype(BF16)
                    return jnp.exp(close[b, h, :, lanes]) * state + kv[b, h, :, lanes].astype(F32)

                lax.fori_loop(0, blocks, advance, came[:, lanes], unroll=4)

    for b in range(PER_TILE):
        rows = slice(b * BLOCK, (b + 1) * BLOCK)
        for h in range(HEADS):
            lanes = slice(h * K, (h + 1) * K)
            both = out[rows, lanes] + nt(q[rows, 2 * h * K : 2 * (h + 1) * K], states[step * PER_TILE + b, h])
            both = both * lax.rsqrt(jnp.mean(both * both, axis=1, keepdims=True) + EPSILON)
            opened = 1.0 + jnp.exp(-gate[rows, lanes].astype(F32))
            recur[rows, lanes] = (both * gain[:, lanes] / opened).astype(BF16)


def finish(arriving, kv, close, q, out, gate, gain):
    rows = q.shape[0]
    whole = lambda a: pl.BlockSpec(a.shape, lambda i: (0,) * a.ndim)
    tile = lambda a: pl.BlockSpec((TILE, a.shape[1]), lambda i: (i, 0))
    return pl.pallas_call(
        finish_kernel,
        grid=(rows // TILE,),
        in_specs=[whole(arriving), whole(kv), whole(close), tile(q), tile(out), tile(gate), whole(gain)],
        out_specs=tile(gate),
        out_shape=jax.ShapeDtypeStruct(gate.shape, BF16),
        scratch_shapes=[pltpu.VMEM(kv.shape, BF16)],
        compiler_params=pltpu.CompilerParams(dimension_semantics=("arbitrary",), vmem_limit_bytes=24 * 2**20),
        name="finish",
    )(arriving, kv, close, q, out, gate, gain)


def around(step):
    return [(i, (i + step) % 4) for i in range(4)]


def up(x):
    return lax.ppermute(x, "tp", around(1))


def down(x):
    return lax.ppermute(x, "tp", around(-1))


def shards(
    tokens,
    norm_gain,
    w_query,
    w_forget_fwd,
    w_forget_bwd,
    w_value,
    w_gate,
    w_pool_in,
    forget_gap,
    added_log_retention,
    initial_state,
    head_gain,
    pool_mix,
    pool_gain,
    w_out_recur,
    w_out_pool,
):
    length = tokens.shape[0]
    tp = lax.axis_index("tp")
    z, y, c = lax.axis_index("z"), lax.axis_index("y"), lax.axis_index("c")
    within = y * 2 + c
    index = z * 8 + within
    weights = (w_query, w_forget_fwd, w_forget_bwd, w_value, w_gate, w_pool_in)
    gain = norm_gain.reshape(4, 1, 512)
    tp_array = tp.astype(jnp.int32).reshape(1)

    near = []
    for first, rows in CHUNKS:
        own = lax.slice_in_dim(tokens, first, first + rows, axis=0)
        near.append((own, up(own), down(own)))
    state = jnp.zeros((HEADS, K, 2 * K), F32)
    total = jnp.zeros((HEADS, 1, 2 * K), F32)
    collected = []
    for (first, rows), (own, left, right) in zip(CHUNKS, near):
        far_a, far_b = up(left[:, :256]), down(right[:, 256:])
        added = lax.slice_in_dim(added_log_retention, first, first + rows, axis=0)
        *chunk, state, total, message = project(
            tp_array, (own, left, right, far_a, far_b), gain, weights, forget_gap, added, state, total
        )
        collected.append(chunk)
    q, k, v, gate, pool_in, kv, close = (jnp.concatenate(a, axis=0) for a in zip(*collected))

    axes = ("z", "y", "c")
    devices = lax.axis_size(axes)
    forward = [(i, i + 1) for i in range(devices - 1)]
    backward = [(j, i) for i, j in forward]
    before = lax.ppermute(pool_in[length - RIM :], axes, forward)
    after = lax.ppermute(pool_in[:RIM], axes, backward)
    blank = jnp.zeros((PAD - RIM, pool_in.shape[1]), BF16)
    padded = jnp.concatenate([blank, before, pool_in, after, blank], axis=0)

    got = lax.all_to_all(message, ("y", "c"), 0, 0, tiled=True)
    prefix, reach, group_message = pl.pallas_call(
        group_kernel,
        out_shape=[
            jax.ShapeDtypeStruct((8, 32, 256), F32),
            jax.ShapeDtypeStruct((8, 32, 256), F32),
            jax.ShapeDtypeStruct((48, 256), BF16),
        ],
        name="group",
    )(got)
    across = lax.all_to_all(jnp.broadcast_to(group_message[None], (8, 48, 256)), "z", 0, 0, tiled=True)
    initial = initial_state.transpose(1, 3, 0, 2).reshape(HEADS, 8, 16, 2 * K)
    initial = lax.dynamic_index_in_dim(initial, within, 1, keepdims=False).reshape(32, 2 * K)
    arriving = pl.pallas_call(
        cross_kernel,
        in_specs=[pl.BlockSpec(memory_space=pltpu.SMEM)] + [pl.BlockSpec(memory_space=pltpu.VMEM)] * 4,
        out_shape=jax.ShapeDtypeStruct((8, 32, 256), BF16),
        name="cross",
    )(z.astype(jnp.int32).reshape(1), across, prefix, reach, initial)
    arriving = lax.all_to_all(arriving, ("y", "c"), 0, 0, tiled=True)

    place = jnp.stack([tp, index * length, jnp.int32(length * devices)]).astype(jnp.int32)
    out, pooled = local(place, q, k, v, padded, pool_mix[0], pool_gain[None])
    recur = finish(arriving, kv, close, q, out, gate, head_gain[None])

    share = length // 4

    def partial(shift):
        at = lax.rem(tp + shift, 4) * share
        a = lax.dynamic_slice_in_dim(recur, at, share, axis=0)
        b = lax.dynamic_slice_in_dim(pooled, at, share, axis=0)
        return nn(a, w_out_recur) + nn(b, w_out_pool)

    half = share // 2
    far = partial(2).astype(BF16)
    came_up, came_down = up(far[:half]), down(far[half:])
    above, below = partial(1), partial(3)
    above_late = up(above[half:].astype(BF16))
    below_late = down(below[:half].astype(BF16))
    above_sum = up((above[:half] + came_up.astype(F32)).astype(BF16))
    below_sum = down((below[half:] + came_down.astype(F32)).astype(BF16))
    own = partial(0)
    top = own[:half] + above_sum.astype(F32) + below_late.astype(F32)
    bottom = own[half:] + above_late.astype(F32) + below_sum.astype(F32)
    return jnp.concatenate([top, bottom], axis=0).astype(BF16)


def solution(mesh):
    split = Mesh(mesh.devices.reshape(8, 4, 2, 4), ("z", "y", "c", "tp"))
    sp = ("z", "y", "c")
    in_specs = (
        P(sp, "tp"),
        P(),
        P(None, "tp"),
        P(None, "tp"),
        P(None, "tp"),
        P(None, "tp"),
        P(None, "tp"),
        P(None, "tp"),
        P(None, "tp"),
        P(sp, "tp"),
        P(None, "tp", None, None),
        P("tp"),
        P("tp", None, None),
        P("tp"),
        P("tp", None),
        P("tp", None),
    )
    out_specs = P(("z", "y", "c", "tp"), None)
    return jax.shard_map(shards, mesh=split, in_specs=in_specs, out_specs=out_specs, check_vma=False)
```
